32 devices in a mesh: grp: 2 (over y), sp: 4 (over z), tp: 4 (over x, core).
Axes of the slice: x: 2, y: 2, z: 4, core: 2. Of those that a mesh axis runs over, the one named last changes fastest.
Arguments:
- stream: bfloat16 [2048, 4096], P(('grp', 'sp'), 'tp'), parts along dimension 0, may hold values from -6 to 6
- gain_pre: float32 [3, 4096], replicated, may hold values from 0.1 to 1.9
- w_in: bfloat16 [3, 4096, 1024], P(None, 'sp', 'tp'), may hold values from -0.09375 to 0.09375
- w_pool: bfloat16 [3, 4, 256, 256], P(None, 'tp'), may hold values from -0.375 to 0.375
- pool_scale: float32 [3, 1024], P(None, 'tp'), may hold values from 0.1 to 1.9
- w_out: bfloat16 [3, 1024, 4096], P(None, 'tp', 'sp'), may hold values from -0.5 to 0.5
- gain_post: float32 [3, 4096], replicated, may hold values from 0.1 to 1.9
Outputs:
- result: bfloat16 [2048, 4096], P(('grp', 'sp'), 'tp'), parts along dimension 0
The draws below stay inside these ranges and needn't reach their ends.
There are 2 independent parts, one for each index of `grp`. The reference program is written for one: setup_inputs(seed, part) draws one part's arguments, and reference() takes and returns one part's arrays. A program takes and returns all parts, laid end to end along the dimension named above; an argument that names none is the same for every part. Nothing has to cross between parts.
All inputs are finite; a program needn't handle non-finite values.
Results may differ from the reference program's by a relative error of at most 0.02.
Values may be sent and summed in bfloat16 or wider, within the bound.
A program may use at most 64 MiB of HBM per device.

```python
import jax
import jax.numpy as jnp
from jax import lax

D = 4096
GROUP = 256
POOL = 1024
LAYERS = 3
TOKENS = 1024


def draw_w_out(key, part):
    key_entries = jax.random.fold_in(key, 11)
    key_rough = jax.random.fold_in(key, 12)
    column_place = jnp.arange(D).astype(jnp.float32) / float(D - 1)
    rough = jax.random.uniform(key_rough, (D,), jnp.float32, 0.7, 1.4)
    entries = jax.random.normal(key_entries, (LAYERS, POOL, D), jnp.float32)
    column_scale = 0.4 * jnp.exp(jnp.log(6.0) * column_place) * rough
    values = entries * column_scale[None, None, :] * float(POOL) ** (-0.5)
    values = jnp.clip(values, -0.5, 0.5)
    return values.astype(jnp.bfloat16)


def block_levels(key, shape, pieces, low, high):
    level = 1.0
    for dim, parts in pieces:
        steps = jax.random.uniform(jax.random.fold_in(jax.random.fold_in(key, 6), dim), (parts,), jnp.float32, low / len(pieces), high / len(pieces))
        level = level * jnp.repeat(jnp.exp(steps), shape[dim] // parts).reshape((-1,) + (1,) * (len(shape) - 1 - dim))
    return level


def gaussian(rng, extent, deviation, most, shards=(), dtype=jnp.bfloat16):
    factor_of = block_levels(rng, extent, shards, -0.22, 0.18) if shards else 1.0
    values = jax.random.normal(rng, extent, jnp.float32) * deviation * factor_of
    return jnp.minimum(jnp.maximum(values, -most), most).astype(dtype)


def setup_inputs(seed: int = 0, part: int = 0) -> dict:
    arg_keys = jax.random.split(jax.random.key(seed), 8)
    part_keys = jax.random.split(jax.random.fold_in(arg_keys[7], part), 8)
    return {
        "stream": gaussian(part_keys[0], (TOKENS, D), 1.0, 6.0, ((0, 4), (1, 4))),
        "gain_pre": jnp.clip(1.0 + 0.18 * jax.random.normal(arg_keys[1], (LAYERS, D), jnp.float32), 0.1, 1.9),
        "w_in": gaussian(arg_keys[2], (LAYERS, D, POOL), D ** -0.5, 0.09375, ((1, 4), (2, 4))),
        "w_pool": gaussian(arg_keys[3], (LAYERS, 4, GROUP, GROUP), GROUP ** -0.5, 0.375, ((1, 4),)),
        "pool_scale": jnp.clip(1.0 + 0.18 * jax.random.normal(arg_keys[4], (LAYERS, POOL), jnp.float32), 0.1, 1.9),
        "w_out": draw_w_out(jax.random.fold_in(arg_keys[7], 71), part),
        "gain_post": jnp.clip(1.0 + 0.18 * jax.random.normal(arg_keys[6], (LAYERS, D), jnp.float32), 0.1, 1.9),
    }


WINDOWS = (2, 4, 8, 16)
EPS = 1e-06

def rms_scale(values, gain):
    inverse = lax.rsqrt(lax.optimization_barrier(jnp.mean(values * values, axis=-1, keepdims=True)) + EPS)
    return values * inverse * gain[None, :]

def reference(stream, gain_pre, w_in, w_pool, pool_scale, w_out, gain_post):
    reach = max(WINDOWS) - 1
    positions = jnp.arange(TOKENS).astype(jnp.float32)
    current = stream
    for layer in range(LAYERS):
        normed = rms_scale(current.astype(jnp.float32), gain_pre[layer]).astype(jnp.bfloat16)
        inner = jnp.dot(normed, w_in[layer], preferred_element_type=jnp.float32).astype(jnp.bfloat16)
        inner_f = inner.astype(jnp.float32)
        padded = jnp.concatenate([jnp.zeros((reach, 4 * GROUP), jnp.float32), inner_f], axis=0)
        branch = jnp.zeros((TOKENS, D), jnp.float32)
        for group_id in range(4):
            window = WINDOWS[group_id]
            lo = group_id * GROUP
            summed = jnp.zeros((TOKENS, GROUP), jnp.float32)
            for offset in range(window):
                summed = summed + padded[reach - offset:reach - offset + TOKENS, lo:lo + GROUP]
            count = jnp.minimum(positions + 1.0, float(window))
            pooled = summed / count[:, None]
            spread = (pooled - inner_f[:, lo:lo + GROUP]).astype(jnp.bfloat16)
            mixed = jnp.dot(spread, w_pool[layer, group_id], preferred_element_type=jnp.float32)
            mixed = (mixed * pool_scale[layer, lo:lo + GROUP][None, :]).astype(jnp.bfloat16)
            partial_value = jnp.dot(mixed, w_out[layer, lo:lo + GROUP], preferred_element_type=jnp.float32)
            partial_value = lax.optimization_barrier(partial_value.astype(jnp.bfloat16))
            branch = branch + partial_value.astype(jnp.float32)
        current = (current.astype(jnp.float32) + rms_scale(branch, gain_post[layer])).astype(jnp.bfloat16)
    return current
```

```python
import functools

import jax
import jax.numpy as jnp
from jax import lax
from jax.experimental import pallas as pl
from jax.experimental.pallas import tpu as pltpu
from jax.sharding import PartitionSpec as P

EPS = 1e-06
HALO = 16
CHUNKS = 4
MESH = pl.DeviceIdType.MESH
F32 = jnp.float32
BF16 = jnp.bfloat16


def kernel(
    G, S, T, layers, width,
    stream, gain_pre, w_in, w_pool, pool_scale, w_out, gain_post,
    out,
    win, wout, ag, part, pair, summed, xgot, normed, acc, ss, branch, ext, halo, sq,
    load_sem, zs_sem, zr_sem, ys_sem, yr_sem,
    agp_sem, agx_sem, agr_sem, ps_sem, pr_sem, xs_sem, xr_sem, qs_sem, qr_sem, hs_sem, hr_sem,
):
    g, s, t = lax.axis_index("grp"), lax.axis_index("sp"), lax.axis_index("tp")
    pairs = T // 2
    p, c = lax.div(t, 2), lax.rem(t, 2)
    mate = p * 2 + 1 - c
    R, F = stream.shape
    group = w_pool.shape[2]
    rows_in, cols_out = w_in.shape[1], w_out.shape[2]
    per = S // T
    step_rows = R // CHUNKS
    use_y = G == 2

    def remote(src, dst, send, recv, where):
        return pltpu.make_async_remote_copy(
            src_ref=src, dst_ref=dst, send_sem=send, recv_sem=recv,
            device_id=where, device_id_type=MESH,
        )

    def span(m, src, which):
        size = rows_in if m % 2 == 0 else group
        small, big = size * 3 // 8, size * 5 // 8
        if not use_y:
            start, length = 0, size
        elif which == "z":
            start, length = g * small, big
        else:
            start, length = g * big, small
        if m % 2 == 0:
            return win.at[m // 2, pl.ds(pl.multiple_of(src * size + start, 16), length), :]
        return wout.at[m // 2, src, pl.ds(pl.multiple_of(start, 16), length), :]

    def z_copy(m, src, way):
        view = span(m, src, "z")
        to = s + 1 if way == 0 else s - 1
        return remote(view, view, zs_sem.at[m, src, way], zr_sem.at[m, src], {"sp": to})

    def y_copy(m, src):
        view = span(m, src, "y")
        return remote(view, view, ys_sem.at[m, src], yr_sem.at[m, src], {"grp": 1 - g})

    def load(m):
        if m % 2 == 0:
            return pltpu.make_async_copy(
                w_in.at[m // 2],
                win.at[m // 2, pl.ds(pl.multiple_of(s * rows_in, 16), rows_in), :],
                load_sem.at[m],
            )
        return pltpu.make_async_copy(w_out.at[m // 2], wout.at[m // 2, s], load_sem.at[m])

    M = 2 * layers

    def own(m):
        if m < M:
            load(m).wait()
            pl.when(s < S - 1)(lambda: z_copy(m, s, 0).start())
            pl.when(s > 0)(lambda: z_copy(m, s, 1).start())

    def relay(m, k):
        def from_left():
            src = s - 1 - k
            z_copy(m, src, 0).wait_recv()
            pl.when(s < S - 1)(lambda: z_copy(m, src, 0).start())
            if use_y:
                y_copy(m, src).start()

        def from_right():
            src = s + 1 + k
            z_copy(m, src, 1).wait_recv()
            pl.when(s > 0)(lambda: z_copy(m, src, 1).start())
            if use_y:
                y_copy(m, src).start()

        pl.when(s - 1 - k >= 0)(from_left)
        pl.when(s + 1 + k <= S - 1)(from_right)

    def pump(m):
        for k in range(S - 1):
            relay(m, k)
            if k == 0:
                own(m + 1)

    def finish(m):
        if use_y:
            for src in range(S):
                pl.when(s != src)(lambda: y_copy(m, src).wait_recv())

    def ag_copy(l, block, j, sem, to):
        view = ag.at[l, block, pl.ds(j * step_rows, step_rows), :]
        return remote(view, view, sem, agr_sem.at[l, block, j], {"tp": to})

    def ag_start(l):
        for j in range(CHUNKS):
            for d in range(1, pairs):
                q = lax.rem(p + d, pairs)
                ag_copy(l, t, j, agx_sem.at[l, q, j], q * 2 + c).start()
        for j in range(CHUNKS):
            ag_copy(l, t, j, agp_sem.at[l, p, j], mate).start()

    def absorb(l, block, first):
        def body(i, carry):
            rows = pl.ds(pl.multiple_of(i * 32, 32), 32)
            x = ag[l, block, rows, :].astype(F32)
            gain = gain_pre[pl.ds(l, 1), pl.ds(pl.multiple_of(block * F, 128), F)]
            square = jnp.broadcast_to(jnp.sum(x * x, axis=1, keepdims=True), (32, 128))
            ss[rows, :] = square if first else ss[rows, :] + square
            normed[rows, :] = (x * gain).astype(BF16)
            return carry

        lax.fori_loop(0, R // 32, body, 0)
        product = jnp.dot(
            normed[...], win[l, pl.ds(pl.multiple_of(block * F, 128), F), :],
            preferred_element_type=F32,
        )
        acc[...] = product if first else acc[...] + product

    def ag_wait(l, block):
        for j in range(CHUNKS):
            ag_copy(l, block, j, agp_sem.at[l, p, j], mate).wait_recv()

    def ag_relay(l):
        for d in range(1, pairs):
            q = lax.rem(p + d, pairs)
            for j in range(CHUNKS):
                copy = ag_copy(l, q * 2 + c, j, agp_sem.at[l, q, j], mate)
                copy.wait_recv()
                copy.start()

    def halo_copy(l):
        return remote(
            ext.at[l, pl.ds(R, HALO), :], halo.at[l], hs_sem.at[l], hr_sem.at[l], {"sp": s + 1}
        )

    def pair_copy(l, q, j):
        rows = pl.ds(j * step_rows, step_rows)
        return remote(
            part.at[l, q * 2 + 1 - c, rows, :], pair.at[l, q, rows, :],
            ps_sem.at[l, q, j], pr_sem.at[l, q, j], {"tp": mate},
        )

    def cross_copy(l, q, j):
        rows = pl.ds(j * step_rows, step_rows)
        return remote(
            summed.at[l, q, rows, :], xgot.at[l, p, rows, :],
            xs_sem.at[l, q, j], xr_sem.at[l, p, j], {"tp": q * 2 + c},
        )

    def cross_wait(l, q, j):
        rows = pl.ds(j * step_rows, step_rows)
        remote(
            summed.at[l, q, rows, :], xgot.at[l, q, rows, :],
            xs_sem.at[l, q, j], xr_sem.at[l, q, j], {"tp": q * 2 + c},
        ).wait_recv()

    def sq_copy(l, slot, to):
        return remote(sq.at[l, slot], sq.at[l, slot], qs_sem.at[l, to], qr_sem.at[l, slot], {"tp": to})

    for m in range(M):
        load(m).start()
    barrier = pltpu.get_barrier_semaphore()

    def greet(where):
        pl.semaphore_signal(barrier, inc=1, device_id=where, device_id_type=MESH)

    pl.when(s < S - 1)(lambda: greet({"sp": s + 1}))
    pl.when(s > 0)(lambda: greet({"sp": s - 1}))
    if use_y:
        greet({"grp": 1 - g})
    for d in range(1, T):
        greet({"tp": lax.rem(t + d, T)})
    ag[0, t] = stream[...]
    ends = jnp.where(s > 0, 1, 0) + jnp.where(s < S - 1, 1, 0)
    pl.semaphore_wait(barrier, ends + (1 if use_y else 0) + T - 1)

    own(0)
    for l in range(layers):
        ag_start(l)
        if l == 0:
            pump(0)
            finish(0)
        else:
            pump(2 * l + 1)
        ag_relay(l)
        if l > 0:
            finish(2 * l)
        absorb(l, t, True)
        ag_wait(l, mate)
        absorb(l, mate, False)
        for d in range(1, pairs):
            q = lax.rem(p + d, pairs)
            absorb(l, q * 2 + c, False)
            ag_wait(l, q * 2 + 1 - c)
            absorb(l, q * 2 + 1 - c, False)
        inverse = lax.rsqrt(ss[:, 0:1] / width + EPS)
        ext[l, pl.ds(HALO, R), :] = (acc[...] * inverse).astype(BF16)
        pl.when(s < S - 1)(lambda: halo_copy(l).start())
        if l == 0:
            pump(1)
        pl.when(s > 0)(lambda: halo_copy(l).wait_recv())

        @pl.when(s == 0)
        def _():
            ext[l, pl.ds(0, HALO), :] = jnp.zeros((HALO, group), BF16)

        @pl.when(s > 0)
        def _():
            ext[l, pl.ds(0, HALO), :] = halo[l]

        values = ext[l].astype(F32)
        two = values + pltpu.roll(values, 1, 0)
        four = two + pltpu.roll(two, 2, 0)
        eight = four + pltpu.roll(four, 4, 0)
        sixteen = eight + pltpu.roll(eight, 8, 0)
        total = jnp.where(t == 0, two, jnp.where(t == 1, four, jnp.where(t == 2, eight, sixteen)))
        window = jnp.where(t == 0, 2, jnp.where(t == 1, 4, jnp.where(t == 2, 8, 16)))
        place = s * R + lax.broadcasted_iota(jnp.int32, (R, group), 0)
        count = jnp.minimum(place + 1, window).astype(F32)
        spread = (total[HALO:, :] / count - values[HALO:, :]).astype(BF16)
        mixed = jnp.dot(spread, w_pool[l, 0], preferred_element_type=F32)
        mixed = (mixed * pool_scale[l : l + 1, :]).astype(BF16)
        finish(2 * l + 1)

        def project(dest):
            for k in range(per):
                value = jnp.dot(mixed, wout[l, dest * per + k], preferred_element_type=F32)
                part[l, dest, :, k * cols_out : (k + 1) * cols_out] = value.astype(BF16)

        for d in range(1, pairs):
            q = lax.rem(p + d, pairs)
            project(q * 2 + 1 - c)
            for j in range(CHUNKS):
                pair_copy(l, q, j).start()
        for d in range(1, pairs):
            q = lax.rem(p + d, pairs)
            project(q * 2 + c)
            for j in range(CHUNKS):
                rows = pl.ds(j * step_rows, step_rows)
                pair_copy(l, q, j).wait_recv()
                summed[l, q, rows, :] = (
                    part[l, q * 2 + c, rows, :].astype(F32) + pair[l, q, rows, :].astype(F32)
                ).astype(BF16)
                cross_copy(l, q, j).start()
        project(mate)
        for j in range(CHUNKS):
            pair_copy(l, p, j).start()
        project(t)
        if l + 1 < layers:
            pump(2 * l + 2)
        for j in range(CHUNKS):
            rows = pl.ds(j * step_rows, step_rows)
            pair_copy(l, p, j).wait_recv()
            for d in range(1, pairs):
                cross_wait(l, lax.rem(p + d, pairs), j)

            def add(i, carry):
                rows = pl.ds(pl.multiple_of(j * step_rows + i * 32, 32), 32)
                value = part[l, t, rows, :].astype(F32) + pair[l, p, rows, :].astype(F32)
                for d in range(1, pairs):
                    value = value + xgot[l, lax.rem(p + d, pairs), rows, :].astype(F32)
                branch[rows, :] = value
                ss[rows, :] = jnp.broadcast_to(jnp.sum(value * value, axis=1, keepdims=True), (32, 128))
                return carry

            lax.fori_loop(0, step_rows // 32, add, 0)
        sq[l, t] = jnp.transpose(ss[...])[0:8, :]
        for d in range(1, T):
            sq_copy(l, t, lax.rem(t + d, T)).start()
        for d in range(1, T):
            other = lax.rem(t + d, T)
            sq_copy(l, other, other).wait_recv()
        squares = sq[l, 0]
        for k in range(1, T):
            squares = squares + sq[l, k]
        inverse = lax.rsqrt(squares / width + EPS)
        ss[...] = jnp.transpose(jnp.concatenate([inverse] * 16, axis=0))

        def update(i, carry):
            rows = pl.ds(pl.multiple_of(i * 32, 32), 32)
            gain = gain_post[pl.ds(l, 1), pl.ds(pl.multiple_of(t * F, 128), F)]
            value = ag[l, t, rows, :].astype(F32) + branch[rows, :] * ss[rows, 0:1] * gain
            if l + 1 < layers:
                ag[l + 1, t, rows, :] = value.astype(BF16)
            else:
                out[rows, :] = value.astype(BF16)
            return carry

        lax.fori_loop(0, R // 32, update, 0)

    for l in range(layers):
        pl.when(s < S - 1)(lambda: halo_copy(l).wait_send())
        for d in range(1, T):
            sq_copy(l, t, lax.rem(t + d, T)).wait_send()
        for j in range(CHUNKS):
            for q in range(pairs):
                ag_copy(l, t, j, agp_sem.at[l, q, j], mate).wait_send()
                pair_copy(l, q, j).wait_send()
            for d in range(1, pairs):
                q = lax.rem(p + d, pairs)
                ag_copy(l, t, j, agx_sem.at[l, q, j], mate).wait_send()
                cross_copy(l, q, j).wait_send()
    for m in range(M):
        for src in range(S):
            pl.when(jnp.logical_and(src <= s, s < S - 1))(lambda: z_copy(m, src, 0).wait_send())
            pl.when(jnp.logical_and(src >= s, s > 0))(lambda: z_copy(m, src, 1).wait_send())
            if use_y:
                pl.when(s != src)(lambda: y_copy(m, src).wait_send())


def per_device(G, S, T, stream, gain_pre, w_in, w_pool, pool_scale, w_out, gain_post):
    layers, width = gain_pre.shape
    R, F = stream.shape
    group = w_pool.shape[2]
    pairs = T // 2
    M = 2 * layers
    dma = pltpu.SemaphoreType.DMA
    vmem = pl.BlockSpec(memory_space=pltpu.VMEM)
    anywhere = pl.BlockSpec(memory_space=pl.ANY)
    return pl.pallas_call(
        functools.partial(kernel, G, S, T, layers, width),
        out_shape=jax.ShapeDtypeStruct((R, F), BF16),
        in_specs=[vmem, vmem, anywhere, vmem, vmem, anywhere, vmem],
        out_specs=vmem,
        scratch_shapes=[
            pltpu.VMEM((layers, width, group), BF16),
            pltpu.VMEM((layers, S, group, w_out.shape[2]), BF16),
            pltpu.VMEM((layers, T, R, F), BF16),
            pltpu.VMEM((layers, T, R, F), BF16),
            pltpu.VMEM((layers, pairs, R, F), BF16),
            pltpu.VMEM((layers, pairs, R, F), BF16),
            pltpu.VMEM((layers, pairs, R, F), BF16),
            pltpu.VMEM((R, F), BF16),
            pltpu.VMEM((R, group), F32),
            pltpu.VMEM((R, 128), F32),
            pltpu.VMEM((R, F), F32),
            pltpu.VMEM((layers, HALO + R, group), BF16),
            pltpu.VMEM((layers, HALO, group), BF16),
            pltpu.VMEM((layers, T, 8, R), F32),
            dma((M,)),
            dma((M, S, 2)),
            dma((M, S)),
            dma((M, S)),
            dma((M, S)),
            dma((layers, pairs, CHUNKS)),
            dma((layers, pairs, CHUNKS)),
            dma((layers, T, CHUNKS)),
            dma((layers, pairs, CHUNKS)),
            dma((layers, pairs, CHUNKS)),
            dma((layers, pairs, CHUNKS)),
            dma((layers, pairs, CHUNKS)),
            dma((layers, T)),
            dma((layers, T)),
            dma((layers,)),
            dma((layers,)),
        ],
        compiler_params=pltpu.CompilerParams(
            collective_id=0, has_side_effects=True, vmem_limit_bytes=60 * 1024 * 1024
        ),
    )(stream, gain_pre, w_in, w_pool, pool_scale, w_out, gain_post)


def solution(mesh):
    G, S, T = mesh.shape["grp"], mesh.shape["sp"], mesh.shape["tp"]
    return jax.shard_map(
        functools.partial(per_device, G, S, T),
        mesh=mesh,
        in_specs=(
            P(("grp", "sp"), "tp"),
            P(),
            P(None, "sp", "tp"),
            P(None, "tp", None, None),
            P(None, "tp"),
            P(None, "tp", "sp"),
            P(),
        ),
        out_specs=P(("grp", "sp"), "tp"),
        check_vma=False,
    )
```

```python
import functools

import jax
import jax.numpy as jnp
from jax import lax
from jax.experimental import pallas as pl
from jax.experimental.pallas import tpu as pltpu
from jax.sharding import PartitionSpec as P

EPS = 1e-06
HALO = 16
CHUNKS = 4
PIECES = 2
MESH = pl.DeviceIdType.MESH
F32 = jnp.float32
BF16 = jnp.bfloat16


def kernel(
    G, S, T, layers, width,
    stream, gain_pre, w_in, w_pool, pool_scale, w_out, gain_post,
    out,
    win, wout, ag, part, pair, summed, xgot, normed, acc, ss, scale, branch, ext, halo, sq,
    load_sem, zs_sem, zr_sem, ys_sem, yr_sem,
    agp_sem, agx_sem, agr_sem, ps_sem, pr_sem, xs_sem, xr_sem, qs_sem, qr_sem, hs_sem, hr_sem,
):
    g, s, t = lax.axis_index("grp"), lax.axis_index("sp"), lax.axis_index("tp")
    pairs = T // 2
    p, c = lax.div(t, 2), lax.rem(t, 2)
    mate = p * 2 + 1 - c
    R, F = stream.shape
    group = w_pool.shape[2]
    rows_in, cols_out = w_in.shape[1], w_out.shape[2]
    per = S // T
    use_y = G == 2

    def remote(src, dst, send, recv, where):
        return pltpu.make_async_remote_copy(
            src_ref=src, dst_ref=dst, send_sem=send, recv_sem=recv,
            device_id=where, device_id_type=MESH,
        )

    def span(m, src, h):
        size = rows_in if m % 2 == 0 else group
        share = size // 2 if use_y else size
        length = share // PIECES
        start = (g * share if use_y else 0) + h * length
        if m % 2 == 0:
            return win.at[m // 2, pl.ds(pl.multiple_of(src * size + start, 16), length), :]
        return wout.at[m // 2, src, pl.ds(pl.multiple_of(start, 16), length), :]

    def z_copy(m, src, way, h):
        view = span(m, src, h)
        to = s + 1 if way == 0 else s - 1
        return remote(view, view, zs_sem.at[m, src, way, h], zr_sem.at[m, src, h], {"sp": to})

    def y_copy(m, src, h):
        view = span(m, src, h)
        return remote(view, view, ys_sem.at[m, src, h], yr_sem.at[m, src, h], {"grp": 1 - g})

    def load(m):
        if m % 2 == 0:
            return pltpu.make_async_copy(
                w_in.at[m // 2],
                win.at[m // 2, pl.ds(pl.multiple_of(s * rows_in, 16), rows_in), :],
                load_sem.at[m],
            )
        return pltpu.make_async_copy(w_out.at[m // 2], wout.at[m // 2, s], load_sem.at[m])

    M = 2 * layers

    def own(m):
        if m < M:
            load(m).wait()
            for h in range(PIECES):
                pl.when(s < S - 1)(lambda: z_copy(m, s, 0, h).start())
                pl.when(s > 0)(lambda: z_copy(m, s, 1, h).start())

    def relay(m, k, h):
        def from_left():
            src = s - 1 - k
            z_copy(m, src, 0, h).wait_recv()
            pl.when(s < S - 1)(lambda: z_copy(m, src, 0, h).start())
            if use_y:
                y_copy(m, src, h).start()

        def from_right():
            src = s + 1 + k
            z_copy(m, src, 1, h).wait_recv()
            pl.when(s > 0)(lambda: z_copy(m, src, 1, h).start())
            if use_y:
                y_copy(m, src, h).start()

        pl.when(s - 1 - k >= 0)(from_left)
        pl.when(s + 1 + k <= S - 1)(from_right)

    units = [(m, k, h) for m in range(M) for k in range(S - 1) for h in range(PIECES)]
    done = [0]

    def tick(n=1):
        for mm, k, h in units[done[0] : done[0] + n]:
            relay(mm, k, h)
            if k == min(1, S - 2) and h == PIECES - 1:
                own(mm + 1)
            done[0] += 1

    def pump(m):
        tick(max(0, (m + 1) * (S - 1) * PIECES - done[0]))

    def finish(m):
        if use_y:
            for src in range(S):
                for h in range(PIECES):
                    pl.when(s != src)(lambda: y_copy(m, src, h).wait_recv())

    def cut(l):
        return R // 2 - HALO * (layers - 1) + HALO * l

    def span_in(l, a):
        return (cut(l), R) if a == 0 else (0, cut(l))

    def span_out(l, a):
        return span_in(l + 1, a)

    def bits(bounds):
        lo, hi = bounds
        mid = lo + ((hi - lo) // 2 + 15) // 16 * 16
        return [(lo, mid), (mid, hi)]

    def sweep(bounds, body):
        lo, hi = bounds
        step = 32 if (hi - lo) % 32 == 0 else 16

        def one(i, carry):
            body(pl.ds(pl.multiple_of(lo + i * step, 16), step))
            return carry

        lax.fori_loop(0, (hi - lo) // step, one, 0)

    def lanes(x):
        return sum(x[:, i : i + 128] for i in range(0, F, 128))

    def ag_copy(l, block, a, i, sem, to):
        lo, hi = bits(span_in(l, a))[i]
        view = ag.at[l, block, pl.ds(lo, hi - lo), :]
        n = a * 2 + i
        return remote(view, view, sem, agr_sem.at[l, block, n], {"tp": to})

    def ag_start(l, a):
        for i in range(2):
            n = a * 2 + i
            for d in range(1, pairs):
                q = lax.rem(p + d, pairs)
                ag_copy(l, t, a, i, agx_sem.at[l, q, n], q * 2 + c).start()
        for i in range(2):
            ag_copy(l, t, a, i, agp_sem.at[l, p, a * 2 + i], mate).start()

    def ag_wait(l, block, a):
        for i in range(2):
            ag_copy(l, block, a, i, agp_sem.at[l, p, a * 2 + i], mate).wait_recv()

    def ag_relay(l, a):
        for d in range(1, pairs):
            q = lax.rem(p + d, pairs)
            for i in range(2):
                copy = ag_copy(l, q * 2 + c, a, i, agp_sem.at[l, q, a * 2 + i], mate)
                copy.wait_recv()
                copy.start()

    def absorb(l, block, a, first):
        lo, hi = span_in(l, a)
        gain = gain_pre[pl.ds(l, 1), pl.ds(pl.multiple_of(block * F, 128), F)]

        def body(rows):
            x = ag[l, block, rows, :].astype(F32)
            square = lanes(x * x)
            ss[rows, :] = square if first else ss[rows, :] + square
            normed[rows, :] = (x * gain).astype(BF16)

        sweep((lo, hi), body)
        product = jnp.dot(
            normed[lo:hi, :], win[l, pl.ds(pl.multiple_of(block * F, 128), F), :],
            preferred_element_type=F32,
        )
        acc[lo:hi, :] = product if first else acc[lo:hi, :] + product

    def inner(l, a):
        lo, hi = span_in(l, a)
        absorb(l, t, a, True)
        ag_wait(l, mate, a)
        absorb(l, mate, a, False)
        for d in range(1, pairs):
            q = lax.rem(p + d, pairs)
            absorb(l, q * 2 + c, a, False)
            ag_wait(l, q * 2 + 1 - c, a)
            absorb(l, q * 2 + 1 - c, a, False)
        inverse = lax.rsqrt(jnp.sum(ss[lo:hi, :], axis=1, keepdims=True) / width + EPS)
        ext[l, HALO + lo : HALO + hi, :] = (acc[lo:hi, :] * inverse).astype(BF16)

    def halo_copy(l):
        return remote(
            ext.at[l, pl.ds(R, HALO), :], halo.at[l], hs_sem.at[l], hr_sem.at[l], {"sp": s + 1}
        )

    def halo_in(l):
        pl.when(s > 0)(lambda: halo_copy(l).wait_recv())

        @pl.when(s == 0)
        def _():
            ext[l, pl.ds(0, HALO), :] = jnp.zeros((HALO, group), BF16)

        @pl.when(s > 0)
        def _():
            ext[l, pl.ds(0, HALO), :] = halo[l]

    def pool(l, a):
        lo, hi = span_out(l, a)
        values = ext[l, lo : hi + HALO, :].astype(F32)
        two = values + pltpu.roll(values, 1, 0)
        four = two + pltpu.roll(two, 2, 0)
        eight = four + pltpu.roll(four, 4, 0)
        sixteen = eight + pltpu.roll(eight, 8, 0)
        total = jnp.where(t == 0, two, jnp.where(t == 1, four, jnp.where(t == 2, eight, sixteen)))
        window = jnp.where(t == 0, 2, jnp.where(t == 1, 4, jnp.where(t == 2, 8, 16)))
        place = s * R + lo + lax.broadcasted_iota(jnp.int32, (hi - lo, group), 0)
        count = jnp.minimum(place + 1, window).astype(F32)
        spread = (total[HALO:, :] / count - values[HALO:, :]).astype(BF16)
        mixed = jnp.dot(spread, w_pool[l, 0], preferred_element_type=F32)
        return (mixed * pool_scale[l : l + 1, :]).astype(BF16)

    def project(l, a, dest, mixed):
        lo, hi = span_out(l, a)
        for k in range(per):
            value = jnp.dot(mixed, wout[l, dest * per + k], preferred_element_type=F32)
            part[l, dest, lo:hi, k * cols_out : (k + 1) * cols_out] = value.astype(BF16)

    def pair_copy(l, q, a, i):
        lo, hi = bits(span_out(l, a))[i]
        rows, n = pl.ds(lo, hi - lo), a * 2 + i
        return remote(
            part.at[l, q * 2 + 1 - c, rows, :], pair.at[l, q, rows, :],
            ps_sem.at[l, q, n], pr_sem.at[l, q, n], {"tp": mate},
        )

    def cross_copy(l, q, slot, a, i):
        lo, hi = bits(span_out(l, a))[i]
        rows, n = pl.ds(lo, hi - lo), a * 2 + i
        return remote(
            summed.at[l, q, rows, :], xgot.at[l, slot, rows, :],
            xs_sem.at[l, q, n], xr_sem.at[l, slot, n], {"tp": q * 2 + c},
        )

    def scatter_first(l, a, mixed):
        for d in range(1, pairs):
            q = lax.rem(p + d, pairs)
            project(l, a, q * 2 + 1 - c, mixed)
            for i in range(2):
                pair_copy(l, q, a, i).start()
        for d in range(1, pairs):
            project(l, a, lax.rem(p + d, pairs) * 2 + c, mixed)

    def scatter_cross(l, a):
        for d in range(1, pairs):
            q = lax.rem(p + d, pairs)
            for i in range(2):
                pair_copy(l, q, a, i).wait_recv()

                def body(rows):
                    summed[l, q, rows, :] = (
                        part[l, q * 2 + c, rows, :].astype(F32) + pair[l, q, rows, :].astype(F32)
                    ).astype(BF16)

                sweep(bits(span_out(l, a))[i], body)
                cross_copy(l, q, p, a, i).start()

    def scatter_own(l, a, mixed):
        project(l, a, mate, mixed)
        for i in range(2):
            pair_copy(l, p, a, i).start()
        project(l, a, t, mixed)

    def sq_copy(l, slot, a, to):
        view = sq.at[l, a, slot]
        return remote(view, view, qs_sem.at[l, a, to], qr_sem.at[l, a, slot], {"tp": to})

    def settle(l, a):
        for i in range(2):
            pair_copy(l, p, a, i).wait_recv()
            for d in range(1, pairs):
                q = lax.rem(p + d, pairs)
                cross_copy(l, q, q, a, i).wait_recv()

            def add(rows):
                value = part[l, t, rows, :].astype(F32) + pair[l, p, rows, :].astype(F32)
                for d in range(1, pairs):
                    value = value + xgot[l, lax.rem(p + d, pairs), rows, :].astype(F32)
                branch[rows, :] = value
                ss[rows, :] = lanes(value * value)

            sweep(bits(span_out(l, a))[i], add)
        row = jnp.sum(jnp.transpose(ss[...]), axis=0, keepdims=True)
        sq[l, a, t] = jnp.broadcast_to(row, (8, R))
        for d in range(1, T):
            sq_copy(l, t, a, lax.rem(t + d, T)).start()
        tick()
        for d in range(1, T):
            other = lax.rem(t + d, T)
            sq_copy(l, other, a, other).wait_recv()
        squares = sq[l, a, 0]
        for k in range(1, T):
            squares = squares + sq[l, a, k]
        inverse = lax.rsqrt(squares / width + EPS)
        scale[...] = jnp.transpose(jnp.concatenate([inverse] * 16, axis=0))
        gain = gain_post[pl.ds(l, 1), pl.ds(pl.multiple_of(t * F, 128), F)]

        def update(rows):
            value = ag[l, t, rows, :].astype(F32) + branch[rows, :] * scale[rows, 0:1] * gain
            if l + 1 < layers:
                ag[l + 1, t, rows, :] = value.astype(BF16)
            else:
                out[rows, :] = value.astype(BF16)

        sweep(span_out(l, a), update)
        if l + 1 < layers:
            ag_start(l + 1, a)

    for m in range(M):
        load(m).start()
    barrier = pltpu.get_barrier_semaphore()

    def greet(where):
        pl.semaphore_signal(barrier, inc=1, device_id=where, device_id_type=MESH)

    pl.when(s < S - 1)(lambda: greet({"sp": s + 1}))
    pl.when(s > 0)(lambda: greet({"sp": s - 1}))
    if use_y:
        greet({"grp": 1 - g})
    for d in range(1, T):
        greet({"tp": lax.rem(t + d, T)})
    ag[0, t] = stream[...]
    ends = jnp.where(s > 0, 1, 0) + jnp.where(s < S - 1, 1, 0)
    pl.semaphore_wait(barrier, ends + (1 if use_y else 0) + T - 1)

    own(0)
    ag_start(0, 0)
    ag_start(0, 1)
    each = (S - 1) * PIECES
    for l in range(layers):
        if l == 0:
            tick(each // 3)
            ag_relay(0, 0)
            tick(each // 3)
            ag_relay(0, 1)
        else:
            ag_relay(l, 0)
        pump(2 * l)
        finish(2 * l)
        inner(l, 0)
        pl.when(s < S - 1)(lambda: halo_copy(l).start())
        mixed = pool(l, 0)
        if l == 0:
            tick()
            inner(l, 1)
            tick()
            halo_in(l)
            later = pool(l, 1)
        pump(2 * l + 1)
        finish(2 * l + 1)
        scatter_first(l, 0, mixed)
        tick()
        if l > 0:
            ag_relay(l, 1)
        scatter_cross(l, 0)
        tick()
        scatter_own(l, 0, mixed)
        tick()
        if l > 0:
            inner(l, 1)
            tick()
            halo_in(l)
            later = pool(l, 1)
        scatter_first(l, 1, later)
        tick()
        scatter_cross(l, 1)
        tick()
        scatter_own(l, 1, later)
        tick()
        settle(l, 0)
        tick()
        settle(l, 1)
        tick()

    for l in range(layers):
        pl.when(s < S - 1)(lambda: halo_copy(l).wait_send())
        for a in range(2):
            for d in range(1, T):
                sq_copy(l, t, a, lax.rem(t + d, T)).wait_send()
            for i in range(2):
                n = a * 2 + i
                for q in range(pairs):
                    ag_copy(l, t, a, i, agp_sem.at[l, q, n], mate).wait_send()
                    pair_copy(l, q, a, i).wait_send()
                for d in range(1, pairs):
                    q = lax.rem(p + d, pairs)
                    ag_copy(l, t, a, i, agx_sem.at[l, q, n], mate).wait_send()
                    cross_copy(l, q, p, a, i).wait_send()
    for m in range(M):
        for src in range(S):
            for h in range(PIECES):
                pl.when(jnp.logical_and(src <= s, s < S - 1))(lambda: z_copy(m, src, 0, h).wait_send())
                pl.when(jnp.logical_and(src >= s, s > 0))(lambda: z_copy(m, src, 1, h).wait_send())
                if use_y:
                    pl.when(s != src)(lambda: y_copy(m, src, h).wait_send())


def per_device(G, S, T, stream, gain_pre, w_in, w_pool, pool_scale, w_out, gain_post):
    layers, width = gain_pre.shape
    R, F = stream.shape
    group = w_pool.shape[2]
    pairs = T // 2
    M = 2 * layers
    dma = pltpu.SemaphoreType.DMA
    vmem = pl.BlockSpec(memory_space=pltpu.VMEM)
    anywhere = pl.BlockSpec(memory_space=pl.ANY)
    return pl.pallas_call(
        functools.partial(kernel, G, S, T, layers, width),
        out_shape=jax.ShapeDtypeStruct((R, F), BF16),
        in_specs=[vmem, vmem, anywhere, vmem, vmem, anywhere, vmem],
        out_specs=vmem,
        scratch_shapes=[
            pltpu.VMEM((layers, width, group), BF16),
            pltpu.VMEM((layers, S, group, w_out.shape[2]), BF16),
            pltpu.VMEM((layers, T, R, F), BF16),
            pltpu.VMEM((layers, T, R, F), BF16),
            pltpu.VMEM((layers, pairs, R, F), BF16),
            pltpu.VMEM((layers, pairs, R, F), BF16),
            pltpu.VMEM((layers, pairs, R, F), BF16),
            pltpu.VMEM((R, F), BF16),
            pltpu.VMEM((R, group), F32),
            pltpu.VMEM((R, 128), F32),
            pltpu.VMEM((R, 128), F32),
            pltpu.VMEM((R, F), F32),
            pltpu.VMEM((layers, HALO + R, group), BF16),
            pltpu.VMEM((layers, HALO, group), BF16),
            pltpu.VMEM((layers, 2, T, 8, R), F32),
            dma((M,)),
            dma((M, S, 2, PIECES)),
            dma((M, S, PIECES)),
            dma((M, S, PIECES)),
            dma((M, S, PIECES)),
            dma((layers, pairs, CHUNKS)),
            dma((layers, pairs, CHUNKS)),
            dma((layers, T, CHUNKS)),
            dma((layers, pairs, CHUNKS)),
            dma((layers, pairs, CHUNKS)),
            dma((layers, pairs, CHUNKS)),
            dma((layers, pairs, CHUNKS)),
            dma((layers, 2, T)),
            dma((layers, 2, T)),
            dma((layers,)),
            dma((layers,)),
        ],
        compiler_params=pltpu.CompilerParams(
            collective_id=0, has_side_effects=True, vmem_limit_bytes=60 * 1024 * 1024
        ),
    )(stream, gain_pre, w_in, w_pool, pool_scale, w_out, gain_post)


def solution(mesh):
    G, S, T = mesh.shape["grp"], mesh.shape["sp"], mesh.shape["tp"]
    return jax.shard_map(
        functools.partial(per_device, G, S, T),
        mesh=mesh,
        in_specs=(
            P(("grp", "sp"), "tp"),
            P(),
            P(None, "sp", "tp"),
            P(None, "tp", None, None),
            P(None, "tp"),
            P(None, "tp", "sp"),
            P(),
        ),
        out_specs=P(("grp", "sp"), "tp"),
        check_vma=False,
    )
```
